32 devices in a mesh: grp: 2 (over y), sp: 4 (over z), tp: 4 (over x, core).
Axes of the slice: x: 2, y: 2, z: 4, core: 2. Of those that a mesh axis runs over, the one named last changes fastest.
Arguments:
- query_rows: bfloat16 [1024, 1024], P(('grp', 'sp'), 'tp'), parts along dimension 0, may hold values from -64 to 64
- key_rows: bfloat16 [1024, 512], P(('grp', 'sp'), 'tp'), parts along dimension 0, may hold values from -16 to 16
- value_rows: bfloat16 [1024, 512], P(('grp', 'sp'), 'tp'), parts along dimension 0, may hold values from -6 to 6
- sink_logit: float32 [16], P('tp'), may hold values from 3.5 to 7
- out_weight: bfloat16 [1024, 2048], P('tp'), may hold values from -0.1875 to 0.1875
- residual: bfloat16 [1024, 2048], P(('grp', 'sp', 'tp')), parts along dimension 0, may hold values from -6 to 6
- norm_gain: float32 [2048], replicated, may hold values from 0.1 to 1.9
- routes: int32 [1024, 6], P(('grp', 'sp', 'tp')), parts along dimension 0, may hold values from 0 to 15, as said below
- gate_weights: float32 [1024, 6], P(('grp', 'sp', 'tp')), parts along dimension 0, may hold values from 0.1 to 0.8
- expert_gate: bfloat16 [16, 2048, 512], P(('sp', 'tp')), may hold values from -0.125 to 0.125
- expert_up: bfloat16 [16, 2048, 512], P(('sp', 'tp')), may hold values from -0.125 to 0.125
- expert_down: bfloat16 [16, 512, 2048], P(('sp', 'tp')), may hold values from -0.25 to 0.25
- shared_gate: bfloat16 [2048, 512], P(None, 'tp'), may hold values from -0.125 to 0.125
- shared_up: bfloat16 [2048, 512], P(None, 'tp'), may hold values from -0.125 to 0.125
- shared_down: bfloat16 [512, 2048], P('tp'), may hold values from -0.25 to 0.25
Outputs:
- layer_out: bfloat16 [1024, 2048], P(('grp', 'sp', 'tp')), parts along dimension 0
The draws below stay inside these ranges and needn't reach their ends.
There are 2 independent parts, one for each index of `grp`. The reference program is written for one: setup_inputs(seed, part) draws one part's arguments, and reference() takes and returns one part's arrays. A program takes and returns all parts, laid end to end along the dimension named above; an argument that names none is the same for every part. Nothing has to cross between parts.
Inputs may be any that keep to these rules, and one draw needn't show every extreme that they name: `routes`: in each aligned block of 32 rows (the rows of one device) every row names 6 different experts and no expert is named by more than 24 rows; in every draw some expert is named by exactly 24 rows of every block.
All inputs are finite; a program needn't handle non-finite values.
Results may differ from the reference program's by a relative error of at most 0.015.
Values may be sent and summed in bfloat16 or wider, within the bound.
No kernel may reach another device: no remote copies, remote signals or barrier semaphores. Data moves between devices by JAX's collectives and lax.ppermute only.
A program may use at most 64 MiB of HBM per device.

```python
import jax
import jax.numpy as jnp
from jax import lax

D = 2048
HEADS = 16
KVH = 8
HEAD = 64
WINDOW = 128
FF = 512
SHARED = 512
TOPK = 6
TOKENS = 512
ROWS = 32
EXPERTS = 16
CAP = 24
N_TP = 4


def plant_pair(key):
    query_key = jax.random.fold_in(key, 101)
    keys_key = jax.random.fold_in(key, 102)
    queries = jnp.clip(jax.random.normal(query_key, (TOKENS, HEADS * HEAD), jnp.float32), -6.0, 6.0)
    keys_all = jnp.clip(jax.random.normal(keys_key, (TOKENS, KVH * HEAD), jnp.float32), -6.0, 6.0)
    return (jnp.clip(queries, -64.0, 64.0), jnp.clip(keys_all, -16.0, 16.0))


def draw_query_rows(key, part):
    return plant_pair(key)[0].astype(jnp.bfloat16)


def draw_key_rows(key, part):
    return plant_pair(key)[1].astype(jnp.bfloat16)


def draw_residual(key, part):
    base_key = jax.random.fold_in(key, 201)
    row_key = jax.random.fold_in(key, 202)
    col_key = jax.random.fold_in(key, 203)
    base_draw = jnp.clip(jax.random.normal(base_key, (TOKENS, D), jnp.float32), -3.5, 3.5)
    row_scale = jnp.exp(jax.random.uniform(row_key, (TOKENS, 1), jnp.float32, jnp.log(0.4), jnp.log(4.0)))
    col_scale = jnp.exp(jax.random.uniform(col_key, (1, D), jnp.float32, jnp.log(0.4), jnp.log(4.0)))
    return (0.1 * base_draw * row_scale * col_scale).astype(jnp.bfloat16)


def draw_routes(key, part):
    block_count = TOKENS // ROWS
    special = jax.random.randint(jax.random.fold_in(key, 7), (), 0, EXPERTS)
    smallest = (CAP + 1) // 2

    def one_block(block_key):
        size_key, perm_key, row_key = jax.random.split(block_key, 3)
        group_size = jax.random.randint(size_key, (EXPERTS,), smallest, CAP + 1).at[0].set(CAP)
        group_end = jnp.cumsum(group_size)
        slot_index = jnp.arange(ROWS * TOPK, dtype=jnp.int32)
        group_of = jnp.sum((group_end[None, :] <= slot_index[:, None]).astype(jnp.int32), axis=1)
        others = jax.random.permutation(perm_key, EXPERTS - 1).astype(jnp.int32) + 1
        mapping = (jnp.concatenate([jnp.zeros((1,), jnp.int32), others]) + special) % EXPERTS
        chosen = mapping[group_of].reshape(TOPK, ROWS).T
        return chosen[jax.random.permutation(row_key, ROWS)]
    blocks_out = jax.vmap(one_block)(jax.random.split(jax.random.fold_in(key, 9), block_count))
    return blocks_out.reshape(TOKENS, TOPK).astype(jnp.int32)


def shard_levels(stream_key, extent, shards, least, top_value):
    def one(axis_at, shards_of):
        draws = jax.random.uniform(jax.random.fold_in(jax.random.fold_in(stream_key, 6), axis_at), (shards_of,), jnp.float32, least / len(shards), top_value / len(shards))
        return jnp.repeat(jnp.exp(draws), extent[axis_at] // shards_of).reshape((-1,) + (1,) * (len(extent) - axis_at - 1))

    level = one(*shards[0])
    for cut in shards[1:]:
        level = level * one(*cut)
    return level


def noise(own_key, dims, scale, reach, shards=(), held_as=jnp.bfloat16):
    array = jax.random.normal(own_key, dims, jnp.float32) * scale
    if len(shards) > 0:
        array = shard_levels(own_key, dims, shards, -0.22, 0.18) * array
    return jnp.clip(array, min=-reach, max=reach).astype(held_as)


def setup_inputs(seed: int = 0, part: int = 0) -> dict:
    streams_of = jax.random.split(jax.random.key(seed), 16)
    part_keys = jax.random.split(jax.random.fold_in(streams_of[15], part), 16)
    query_rows = draw_query_rows(jax.random.fold_in(jax.random.fold_in(streams_of[15], part), 71), part)
    key_rows = draw_key_rows(jax.random.fold_in(jax.random.fold_in(streams_of[15], part), 71), part)
    value_rows = noise(part_keys[2], (TOKENS, KVH * HEAD), 1.0, 6.0, ((0, 4), (1, 4)))
    sink_logit = jnp.clip(3.5 + 3.5 * jax.random.uniform(streams_of[3], (HEADS,), jnp.float32) ** shard_levels(streams_of[3], (HEADS,), ((0, 4),), -0.2, 0.2), 3.5, 7.0)
    out_weight = noise(streams_of[4], (HEADS * HEAD, D), (HEADS * HEAD) ** -0.5, 0.1875, ((0, 4),))
    residual = draw_residual(jax.random.fold_in(jax.random.fold_in(streams_of[15], part), 71), part)
    norm_gain = jnp.clip(1.0 + 0.18 * jax.random.normal(streams_of[6], (D,), jnp.float32), 0.1, 1.9)
    routes = draw_routes(jax.random.fold_in(jax.random.fold_in(streams_of[15], part), 71), part)
    gate_weights = jnp.clip(0.1 + 0.7 * jax.random.uniform(part_keys[8], (TOKENS, TOPK), jnp.float32) ** shard_levels(part_keys[8], (TOKENS, TOPK), ((0, 16),), -0.2, 0.2), 0.1, 0.8)
    expert_gate = noise(streams_of[9], (EXPERTS, D, FF), D ** -0.5, 0.125, ((0, 16),))
    expert_up = noise(streams_of[10], (EXPERTS, D, FF), D ** -0.5, 0.125, ((0, 16),))
    expert_down = noise(streams_of[11], (EXPERTS, FF, D), FF ** -0.5, 0.25, ((0, 16),))
    shared_gate = noise(streams_of[12], (D, SHARED), D ** -0.5, 0.125, ((1, 4),))
    shared_up = noise(streams_of[13], (D, SHARED), D ** -0.5, 0.125, ((1, 4),))
    shared_down = noise(streams_of[14], (SHARED, D), SHARED ** -0.5, 0.25, ((0, 4),))
    return {"query_rows": query_rows, "key_rows": key_rows, "value_rows": value_rows, "sink_logit": sink_logit, "out_weight": out_weight, "residual": residual, "norm_gain": norm_gain, "routes": routes, "gate_weights": gate_weights, "expert_gate": expert_gate, "expert_up": expert_up, "expert_down": expert_down, "shared_gate": shared_gate, "shared_up": shared_up, "shared_down": shared_down}


norm_eps = 1e-06

def band_view(tensor, blocks):
    shaped = tensor.reshape(blocks, WINDOW, tensor.shape[1], tensor.shape[2])
    padded = jnp.pad(shaped, ((1, 1), (0, 0), (0, 0), (0, 0)))
    return jnp.concatenate([padded[:-2], padded[1:-1], padded[2:]], axis=1)

def attention(query_rows, key_rows, value_rows, sink_logit):
    length = query_rows.shape[0]
    blocks = length // WINDOW
    groups = HEADS // KVH
    queries = query_rows.astype(jnp.float32).reshape(blocks, WINDOW, KVH, groups, HEAD)
    keyband = band_view(key_rows.astype(jnp.float32).reshape(length, KVH, HEAD), blocks)
    valband = band_view(value_rows.astype(jnp.float32).reshape(length, KVH, HEAD), blocks)
    block_ids = jnp.arange(blocks, dtype=jnp.int32)[:, None, None]
    query_pos = block_ids * WINDOW + jnp.arange(WINDOW, dtype=jnp.int32)[None, :, None]
    key_pos = (block_ids - 1) * WINDOW + jnp.arange(3 * WINDOW, dtype=jnp.int32)[None, None, :]
    in_window = (jnp.abs(key_pos - query_pos) <= WINDOW) & (key_pos >= 0) & (key_pos < length)

    def one_head(head_index):
        query_part = queries[:, :, head_index]
        key_part = keyband[:, :, head_index]
        value_part = valband[:, :, head_index]
        scores = jnp.einsum('nqgd,nkd->ngqk', query_part, key_part) * HEAD ** (-0.5)
        scores = jnp.where(in_window[:, None], scores, -jnp.inf)
        sink_part = lax.dynamic_slice_in_dim(sink_logit, head_index * groups, groups).reshape(1, groups, 1, 1)
        row_max = jnp.maximum(sink_part, lax.optimization_barrier(jnp.max(scores, axis=-1, keepdims=True)))
        shifted = jnp.exp(scores - row_max)
        denominator = jnp.exp(sink_part - row_max) + lax.optimization_barrier(jnp.sum(shifted, axis=-1, keepdims=True))
        weights = lax.optimization_barrier((shifted / denominator).astype(jnp.bfloat16))
        weighted = jnp.einsum('ngqk,nkd->nqgd', weights.astype(jnp.float32), value_part)
        return weighted.astype(jnp.bfloat16)
    heads_out = lax.map(one_head, jnp.arange(KVH, dtype=jnp.int32))
    return jnp.transpose(heads_out, (1, 2, 0, 3, 4)).reshape(length, HEADS * HEAD)

def routed_experts(normed, routes, gate_weights, expert_gate, expert_up, expert_down):
    tokens = normed.shape[0]
    model_width = normed.shape[1]
    copies = tokens * TOPK
    block_rows = 64
    flat_expert = routes.reshape(-1).astype(jnp.int32)
    order_index = jnp.argsort(flat_expert, stable=True).astype(jnp.int32)
    sorted_expert = flat_expert[order_index]
    counts = jax.ops.segment_sum(jnp.ones((copies,), jnp.int32), flat_expert, num_segments=EXPERTS)
    padded_counts = (counts + block_rows - 1) // block_rows * block_rows
    padded_end = jnp.cumsum(padded_counts).astype(jnp.int32)
    padded_start = padded_end - padded_counts
    group_start = (jnp.cumsum(counts) - counts).astype(jnp.int32)
    target = padded_start[sorted_expert] + jnp.arange(copies, dtype=jnp.int32) - group_start[sorted_expert]
    block_count = (copies + EXPERTS * (block_rows - 1) + block_rows - 1) // block_rows
    slot_copy = jnp.full((block_count * block_rows,), copies, jnp.int32).at[target].set(order_index)
    block_first = jnp.arange(block_count, dtype=jnp.int32) * block_rows
    block_expert = jnp.minimum(jnp.searchsorted(padded_end, block_first, side='right'), EXPERTS - 1).astype(jnp.int32)
    copy_token = jnp.concatenate([jnp.arange(copies, dtype=jnp.int32) // TOPK, jnp.full((1,), tokens, jnp.int32)])
    padded_rows = jnp.concatenate([normed, jnp.zeros((1, model_width), normed.dtype)], axis=0)

    def run_block(inputs):
        slot_ids, expert_id = inputs
        block_in = padded_rows[copy_token[slot_ids]]
        gate_part = jnp.dot(block_in, expert_gate[expert_id], preferred_element_type=jnp.float32)
        up_part = jnp.dot(block_in, expert_up[expert_id], preferred_element_type=jnp.float32)
        hidden = (jax.nn.silu(gate_part) * up_part).astype(jnp.bfloat16)
        return jnp.dot(hidden, expert_down[expert_id], preferred_element_type=jnp.float32).astype(jnp.bfloat16)
    outputs = lax.map(run_block, (slot_copy.reshape(block_count, block_rows), block_expert))
    per_copy = jnp.zeros((copies + 1, model_width), jnp.bfloat16).at[slot_copy].set(outputs.reshape(-1, model_width))
    per_copy = lax.optimization_barrier(per_copy[:copies].reshape(tokens, TOPK, model_width))
    return lax.optimization_barrier(jnp.sum(gate_weights[:, :, None] * per_copy.astype(jnp.float32), axis=1))

def shared_expert(normed, shared_gate, shared_up, shared_down):
    gate_part = jnp.dot(normed, shared_gate, preferred_element_type=jnp.float32)
    up_part = jnp.dot(normed, shared_up, preferred_element_type=jnp.float32)
    hidden = (jax.nn.silu(gate_part) * up_part).astype(jnp.bfloat16)
    unit_count = SHARED // N_TP
    totals = jnp.zeros((normed.shape[0], shared_down.shape[1]), jnp.float32)
    for group_index in range(N_TP):
        lower_unit = group_index * unit_count
        partial_sum = jnp.dot(hidden[:, lower_unit:lower_unit + unit_count], shared_down[lower_unit:lower_unit + unit_count], preferred_element_type=jnp.float32)
        totals = totals + lax.optimization_barrier(partial_sum.astype(jnp.bfloat16)).astype(jnp.float32)
    return totals

def reference(query_rows, key_rows, value_rows, sink_logit, out_weight, residual, norm_gain, routes, gate_weights, expert_gate, expert_up, expert_down, shared_gate, shared_up, shared_down):
    attended = attention(query_rows, key_rows, value_rows, sink_logit)
    projected = jnp.dot(attended, out_weight, preferred_element_type=jnp.float32)
    stream = residual.astype(jnp.float32) + projected
    normed = (stream * lax.rsqrt(lax.optimization_barrier(jnp.mean(stream * stream, axis=-1, keepdims=True)) + norm_eps) * norm_gain).astype(jnp.bfloat16)
    routed = routed_experts(normed, routes, gate_weights, expert_gate, expert_up, expert_down)
    shared = shared_expert(normed, shared_gate, shared_up, shared_down)
    return (stream + routed + shared).astype(jnp.bfloat16)
```

```python
import jax
import jax.numpy as jnp
from jax import lax
from jax.sharding import PartitionSpec as P

HEAD = 64
WINDOW = 128
TOPK = 6
LANES = 128

norm_eps = 1e-06


def with_halo(block, sides, width):
    for axis, dim in sides:
        count = lax.axis_size(axis)
        forward = [(i, i + 1) for i in range(count - 1)]
        backward = [(target, source) for source, target in forward]
        low = lax.ppermute(
            lax.slice_in_dim(block, block.shape[dim] - width, None, axis=dim), axis, forward
        )
        high = lax.ppermute(lax.slice_in_dim(block, 0, width, axis=dim), axis, backward)
        block = jnp.concatenate([low, block, high], axis=dim)
    return block


def window_attention(query_rows, key_rows, value_rows, sink_logit):
    local_len = query_rows.shape[0]
    head_size = HEAD
    local_kv = key_rows.shape[1] // head_size
    local_heads = query_rows.shape[1] // head_size
    grouped = local_heads // local_kv
    blocks = local_len // WINDOW
    stacked = jnp.stack([key_rows, value_rows])
    widened = with_halo(stacked, (("sp", 1),), WINDOW)
    banded = widened.reshape(2, blocks + 2, WINDOW, local_kv, head_size)
    banded = jnp.concatenate([banded[:, :-2], banded[:, 1:-1], banded[:, 2:]], axis=2)
    queries = query_rows.reshape(blocks, WINDOW, local_kv, grouped, head_size)
    scores = jnp.einsum(
        "nqhgd,nkhd->nhgqk", queries, banded[0], preferred_element_type=jnp.float32
    ) * head_size ** (-0.5)
    seq_start = lax.axis_index("sp") * local_len
    total_len = lax.axis_size("sp") * local_len
    block_ids = jnp.arange(blocks, dtype=jnp.int32)[:, None, None]
    query_pos = seq_start + block_ids * WINDOW + jnp.arange(WINDOW, dtype=jnp.int32)[None, :, None]
    key_pos = (
        seq_start
        + (block_ids - 1) * WINDOW
        + jnp.arange(3 * WINDOW, dtype=jnp.int32)[None, None, :]
    )
    in_window = (jnp.abs(key_pos - query_pos) <= WINDOW) & (key_pos >= 0) & (key_pos < total_len)
    scores = jnp.where(in_window[:, None, None], scores, -jnp.inf)
    sink_part = sink_logit.reshape(1, local_kv, grouped, 1, 1)
    row_max = jnp.maximum(sink_part, jnp.max(scores, axis=-1, keepdims=True))
    shifted = jnp.exp(scores - row_max)
    denominator = jnp.exp(sink_part - row_max) + jnp.sum(shifted, axis=-1, keepdims=True)
    weights = (shifted / denominator).astype(jnp.bfloat16)
    attended = jnp.einsum(
        "nhgqk,nkhd->nqhgd", weights, banded[1], preferred_element_type=jnp.float32
    )
    return attended.astype(jnp.bfloat16).reshape(local_len, local_heads * head_size)


def rms_norm(stream, norm_gain):
    return (
        stream * lax.rsqrt(jnp.mean(stream * stream, axis=-1, keepdims=True) + norm_eps) * norm_gain
    ).astype(jnp.bfloat16)


def gated(rows, gate, up):
    gate_part = jnp.dot(rows, gate, preferred_element_type=jnp.float32)
    up_part = jnp.dot(rows, up, preferred_element_type=jnp.float32)
    return (jax.nn.silu(gate_part) * up_part).astype(jnp.bfloat16)


def dispatched_layer(attended, operands):
    out_weight, residual, norm_gain, routes, gate_weights = operands[:5]
    expert_gate, expert_up, expert_down, shared_gate, shared_up, shared_down = operands[5:]
    tok_dev = attended.shape[0]
    tok_rows = residual.shape[0]
    model_width = residual.shape[1]
    projected = lax.psum_scatter(
        jnp.dot(attended, out_weight, preferred_element_type=jnp.float32).astype(jnp.bfloat16),
        "tp",
        scatter_dimension=0,
        tiled=True,
    ).astype(jnp.float32)
    stream = residual.astype(jnp.float32) + projected
    normed = rms_norm(stream, norm_gain)
    sp_count = lax.axis_size("sp")
    tp_count = lax.axis_size("tp")
    experts_all = sp_count * tp_count
    capacity = (2 * tok_dev * TOPK + tp_count * experts_all - 1) // (tp_count * experts_all)
    copies = tok_rows * TOPK
    flat_expert = routes.reshape(-1)
    one_hot = (flat_expert[:, None] == jnp.arange(experts_all, dtype=jnp.int32)[None, :]).astype(
        jnp.int32
    )
    rank_in_expert = jnp.sum(jnp.cumsum(one_hot, axis=0) * one_hot, axis=1) - 1
    target_slot = flat_expert * capacity + rank_in_expert
    slot_token = (
        jnp.full((experts_all * capacity,), tok_rows, jnp.int32)
        .at[target_slot]
        .set(jnp.arange(copies, dtype=jnp.int32) // TOPK)
    )
    padded_rows = jnp.concatenate([normed, jnp.zeros((1, model_width), jnp.bfloat16)], axis=0)
    outgoing = padded_rows[slot_token].reshape(experts_all, capacity, model_width)
    incoming = lax.all_to_all(outgoing, ("sp", "tp"), split_axis=0, concat_axis=0, tiled=True)
    hidden = gated(incoming.reshape(-1, model_width), expert_gate[0], expert_up[0])
    result = jnp.dot(hidden, expert_down[0], preferred_element_type=jnp.float32).astype(
        jnp.bfloat16
    )
    returned = lax.all_to_all(
        result.reshape(incoming.shape), ("sp", "tp"), split_axis=0, concat_axis=0, tiled=True
    )
    returned = returned.reshape(experts_all * capacity, model_width)
    gathered_copies = returned[target_slot].reshape(tok_rows, TOPK, model_width)
    routed = jnp.sum(gate_weights[:, :, None] * gathered_copies.astype(jnp.float32), axis=1)
    slab_rows = lax.all_gather(normed, "tp", axis=0, tiled=True)
    hidden = gated(slab_rows, shared_gate, shared_up)
    partials = jnp.dot(hidden, shared_down, preferred_element_type=jnp.float32)
    shared = lax.psum_scatter(
        partials.astype(jnp.bfloat16), "tp", scatter_dimension=0, tiled=True
    ).astype(jnp.float32)
    return (stream + routed + shared).astype(jnp.bfloat16)


def flip(value, bit):
    count = lax.axis_size("tp")
    return lax.ppermute(value, "tp", [(i, i ^ bit) for i in range(count)])


def turn(value, step):
    count = lax.axis_size("sp")
    return lax.ppermute(value, "sp", [(i, (i + step) % count) for i in range(count)])


def gathered_layer(attended, operands):
    out_weight, residual, norm_gain, routes, gate_weights = operands[:5]
    expert_gate, expert_up, expert_down, shared_gate, shared_up, shared_down = operands[5:]
    tok_rows, model_width = residual.shape
    sp_count = lax.axis_size("sp")
    experts_all = sp_count * lax.axis_size("tp")
    me = lax.axis_index("tp")

    def block_of(peer):
        return lax.dynamic_slice_in_dim(attended, (me ^ peer) * tok_rows, tok_rows, axis=0)

    def project(first, second):
        rows = jnp.concatenate([block_of(first), block_of(second)], axis=0)
        return jnp.dot(rows, out_weight, preferred_element_type=jnp.float32)

    from_sibling = flip(project(1, 3).astype(jnp.bfloat16), 1)
    pair_sum = project(0, 2) + from_sibling.astype(jnp.float32)
    from_peer = flip(pair_sum[tok_rows:].astype(jnp.bfloat16), 2)
    stream = residual.astype(jnp.float32) + pair_sum[:tok_rows] + from_peer.astype(jnp.float32)
    normed = rms_norm(stream, norm_gain)

    expert_ids = jnp.arange(experts_all, dtype=jnp.int32)
    dense = jnp.sum(
        jnp.where(routes[:, :, None] == expert_ids, gate_weights[:, :, None], 0.0), axis=1
    )
    dense_high = dense.astype(jnp.bfloat16)
    dense_low = (dense - dense_high.astype(jnp.float32)).astype(jnp.bfloat16)
    spare = -(2 * experts_all) % LANES
    payload = jnp.concatenate(
        [normed, dense_high, dense_low, jnp.zeros((tok_rows, spare), jnp.bfloat16)], axis=1
    )
    my_expert = lax.axis_index("sp") * lax.axis_size("tp") + me
    lane = jnp.arange(2 * experts_all + spare, dtype=jnp.int32)
    mine = (lane == my_expert) | (lane == my_expert + experts_all)

    straight = [payload] + [turn(payload, step) for step in range(1, sp_count)]
    crossed = [flip(rows, 2) for rows in straight]
    slabs = []
    for rows, other in zip(straight, crossed):
        both = jnp.concatenate([rows, other], axis=0)
        slabs.append(jnp.concatenate([both, flip(both, 1)], axis=0))

    def expert_part(slab):
        rows = slab[:, :model_width]
        weight = jnp.sum(
            jnp.where(mine, slab[:, model_width:].astype(jnp.float32), 0.0), axis=1, keepdims=True
        )
        hidden = gated(rows, expert_gate[0], expert_up[0])
        result = jnp.dot(hidden, expert_down[0], preferred_element_type=jnp.float32)
        return weight * result.astype(jnp.bfloat16).astype(jnp.float32)

    def returned(part):
        half = 2 * tok_rows
        kept = part[:half] + flip(part[half:].astype(jnp.bfloat16), 1).astype(jnp.float32)
        crossed_back = flip(kept[tok_rows:].astype(jnp.bfloat16), 2).astype(jnp.float32)
        return kept[:tok_rows] + crossed_back

    total = stream
    for step in range(1, sp_count):
        part = returned(expert_part(slabs[step])).astype(jnp.bfloat16)
        total = total + turn(part, -step).astype(jnp.float32)
    own = slabs[0]
    hidden = gated(own[:, :model_width], shared_gate, shared_up)
    shared = jnp.dot(hidden, shared_down, preferred_element_type=jnp.float32)
    shared = shared.astype(jnp.bfloat16).astype(jnp.float32)
    total = total + returned(expert_part(own) + shared)
    return total.astype(jnp.bfloat16)


def body(query_rows, key_rows, value_rows, sink_logit, *operands):
    attended = window_attention(query_rows, key_rows, value_rows, sink_logit)
    sp_count = lax.axis_size("sp")
    tp_count = lax.axis_size("tp")
    experts_all = sp_count * tp_count
    rows_all = sp_count * attended.shape[0]
    sent = 2 * operands[1].shape[0] * TOPK
    if tp_count == 4 and 2 * sent >= rows_all:
        return gathered_layer(attended, operands)
    return dispatched_layer(attended, operands)


def solution(mesh):
    placed = (
        P(("grp", "sp"), "tp"),
        P(("grp", "sp"), "tp"),
        P(("grp", "sp"), "tp"),
        P("tp"),
        P("tp", None),
        P(("grp", "sp", "tp"), None),
        P(),
        P(("grp", "sp", "tp"), None),
        P(("grp", "sp", "tp"), None),
        P(("sp", "tp"), None, None),
        P(("sp", "tp"), None, None),
        P(("sp", "tp"), None, None),
        P(None, "tp"),
        P(None, "tp"),
        P("tp", None),
    )
    return jax.shard_map(
        body, mesh=mesh, in_specs=placed, out_specs=P(("grp", "sp", "tp"), None), check_vma=False
    )
```

```python
import functools

import jax
import jax.numpy as jnp
from jax import lax
from jax.experimental import pallas as pl
from jax.experimental.pallas import tpu as pltpu
from jax.sharding import PartitionSpec as P

HEAD = 64
WINDOW = 128
TOPK = 6
LANES = 128
VMEM_BYTES = 12 * 1024 * 1024

norm_eps = 1e-06


def with_halo(block, sides, width):
    for axis, dim in sides:
        count = lax.axis_size(axis)
        forward = [(i, i + 1) for i in range(count - 1)]
        backward = [(target, source) for source, target in forward]
        low = lax.ppermute(
            lax.slice_in_dim(block, block.shape[dim] - width, None, axis=dim), axis, forward
        )
        high = lax.ppermute(lax.slice_in_dim(block, 0, width, axis=dim), axis, backward)
        block = jnp.concatenate([low, block, high], axis=dim)
    return block


def window_attention(query_rows, key_rows, value_rows, sink_logit):
    local_len = query_rows.shape[0]
    head_size = HEAD
    local_kv = key_rows.shape[1] // head_size
    local_heads = query_rows.shape[1] // head_size
    grouped = local_heads // local_kv
    blocks = local_len // WINDOW
    stacked = jnp.stack([key_rows, value_rows])
    widened = with_halo(stacked, (("sp", 1),), WINDOW)
    banded = widened.reshape(2, blocks + 2, WINDOW, local_kv, head_size)
    banded = jnp.concatenate([banded[:, :-2], banded[:, 1:-1], banded[:, 2:]], axis=2)
    queries = query_rows.reshape(blocks, WINDOW, local_kv, grouped, head_size)
    scores = jnp.einsum(
        "nqhgd,nkhd->nhgqk", queries, banded[0], preferred_element_type=jnp.float32
    ) * head_size ** (-0.5)
    seq_start = lax.axis_index("sp") * local_len
    total_len = lax.axis_size("sp") * local_len
    block_ids = jnp.arange(blocks, dtype=jnp.int32)[:, None, None]
    query_pos = seq_start + block_ids * WINDOW + jnp.arange(WINDOW, dtype=jnp.int32)[None, :, None]
    key_pos = (
        seq_start
        + (block_ids - 1) * WINDOW
        + jnp.arange(3 * WINDOW, dtype=jnp.int32)[None, None, :]
    )
    in_window = (jnp.abs(key_pos - query_pos) <= WINDOW) & (key_pos >= 0) & (key_pos < total_len)
    scores = jnp.where(in_window[:, None, None], scores, -jnp.inf)
    sink_part = sink_logit.reshape(1, local_kv, grouped, 1, 1)
    row_max = jnp.maximum(sink_part, jnp.max(scores, axis=-1, keepdims=True))
    shifted = jnp.exp(scores - row_max)
    denominator = jnp.exp(sink_part - row_max) + jnp.sum(shifted, axis=-1, keepdims=True)
    weights = (shifted / denominator).astype(jnp.bfloat16)
    attended = jnp.einsum(
        "nhgqk,nkhd->nqhgd", weights, banded[1], preferred_element_type=jnp.float32
    )
    return attended.astype(jnp.bfloat16).reshape(local_len, local_heads * head_size)


def rms_norm(stream, norm_gain):
    return (
        stream * lax.rsqrt(jnp.mean(stream * stream, axis=-1, keepdims=True) + norm_eps) * norm_gain
    ).astype(jnp.bfloat16)


def gated(rows, gate, up):
    gate_part = jnp.dot(rows, gate, preferred_element_type=jnp.float32)
    up_part = jnp.dot(rows, up, preferred_element_type=jnp.float32)
    return (jax.nn.silu(gate_part) * up_part).astype(jnp.bfloat16)


def dispatched_layer(attended, operands):
    out_weight, residual, norm_gain, routes, gate_weights = operands[:5]
    expert_gate, expert_up, expert_down, shared_gate, shared_up, shared_down = operands[5:]
    tok_dev = attended.shape[0]
    tok_rows = residual.shape[0]
    model_width = residual.shape[1]
    projected = lax.psum_scatter(
        jnp.dot(attended, out_weight, preferred_element_type=jnp.float32).astype(jnp.bfloat16),
        "tp",
        scatter_dimension=0,
        tiled=True,
    ).astype(jnp.float32)
    stream = residual.astype(jnp.float32) + projected
    normed = rms_norm(stream, norm_gain)
    sp_count = lax.axis_size("sp")
    tp_count = lax.axis_size("tp")
    experts_all = sp_count * tp_count
    capacity = (2 * tok_dev * TOPK + tp_count * experts_all - 1) // (tp_count * experts_all)
    copies = tok_rows * TOPK
    flat_expert = routes.reshape(-1)
    one_hot = (flat_expert[:, None] == jnp.arange(experts_all, dtype=jnp.int32)[None, :]).astype(
        jnp.int32
    )
    rank_in_expert = jnp.sum(jnp.cumsum(one_hot, axis=0) * one_hot, axis=1) - 1
    target_slot = flat_expert * capacity + rank_in_expert
    slot_token = (
        jnp.full((experts_all * capacity,), tok_rows, jnp.int32)
        .at[target_slot]
        .set(jnp.arange(copies, dtype=jnp.int32) // TOPK)
    )
    padded_rows = jnp.concatenate([normed, jnp.zeros((1, model_width), jnp.bfloat16)], axis=0)
    outgoing = padded_rows[slot_token].reshape(experts_all, capacity, model_width)
    incoming = lax.all_to_all(outgoing, ("sp", "tp"), split_axis=0, concat_axis=0, tiled=True)
    hidden = gated(incoming.reshape(-1, model_width), expert_gate[0], expert_up[0])
    result = jnp.dot(hidden, expert_down[0], preferred_element_type=jnp.float32).astype(
        jnp.bfloat16
    )
    returned = lax.all_to_all(
        result.reshape(incoming.shape), ("sp", "tp"), split_axis=0, concat_axis=0, tiled=True
    )
    returned = returned.reshape(experts_all * capacity, model_width)
    gathered_copies = returned[target_slot].reshape(tok_rows, TOPK, model_width)
    routed = jnp.sum(gate_weights[:, :, None] * gathered_copies.astype(jnp.float32), axis=1)
    slab_rows = lax.all_gather(normed, "tp", axis=0, tiled=True)
    hidden = gated(slab_rows, shared_gate, shared_up)
    partials = jnp.dot(hidden, shared_down, preferred_element_type=jnp.float32)
    shared = lax.psum_scatter(
        partials.astype(jnp.bfloat16), "tp", scatter_dimension=0, tiled=True
    ).astype(jnp.float32)
    return (stream + routed + shared).astype(jnp.bfloat16)


def dot32(left, right):
    return jnp.dot(left, right, preferred_element_type=jnp.float32)


def later(index):
    return ((index + 1) ^ 1) - 1


def attention_kernel(total_len, given, sources, results, arrival):
    place_ref, sink_ref = given
    kept_ref, sent_ref, attended_ref, query_ref, keys_ref, values_ref, weight_ref = results
    rows = query_ref.shape[0]
    keys = [keys_ref.at[pl.ds(index * rows, rows)] for index in range(3)]
    values = [values_ref.at[pl.ds(index * rows, rows)] for index in range(3)]
    copies = fetch(sources, [query_ref, *keys, *values, weight_ref], arrival)
    heads = query_ref.shape[1] // HEAD
    kv_heads = keys_ref.shape[1] // HEAD
    grouped = heads // kv_heads
    here, me = place_ref[0], place_ref[1]
    span = (grouped * rows, 3 * rows)
    row = lax.broadcasted_iota(jnp.int32, span, 0)
    col = lax.broadcasted_iota(jnp.int32, span, 1)
    first = jnp.where(col < 2 * rows, ((here ^ 1) - 1) * rows, (later(here) - 2) * rows)
    key_pos = col + jnp.where(col < rows, here * rows, first)
    query_pos = here * rows + row % rows
    near = (jnp.abs(key_pos - query_pos) <= WINDOW) & (key_pos >= 0) & (key_pos < total_len)
    head_of = row[:, :1] // rows
    for copy in copies[:-1]:
        copy.wait()
    for group in range(kv_heads):
        lanes = slice(group * HEAD, (group + 1) * HEAD)
        first_head = group * grouped
        queries = jnp.concatenate(
            [
                query_ref[:, head * HEAD : (head + 1) * HEAD]
                for head in range(first_head, first_head + grouped)
            ],
            axis=0,
        )
        scores = lax.dot_general(
            queries, keys_ref[:, lanes], (((1,), (1,)), ((), ())), preferred_element_type=jnp.float32
        )
        scores = jnp.where(near, scores * HEAD ** (-0.5), -jnp.inf)
        sink = jnp.full(head_of.shape, sink_ref[first_head], jnp.float32)
        for offset in range(1, grouped):
            sink = jnp.where(head_of == offset, sink_ref[first_head + offset], sink)
        row_max = jnp.maximum(sink, jnp.max(scores, axis=1, keepdims=True))
        shifted = jnp.exp(scores - row_max)
        denominator = jnp.exp(sink - row_max) + jnp.sum(shifted, axis=1, keepdims=True)
        weights = (shifted / denominator).astype(jnp.bfloat16)
        out = dot32(weights, values_ref[:, lanes]).astype(jnp.bfloat16)
        for offset in range(grouped):
            head = first_head + offset
            attended_ref[:, head * HEAD : (head + 1) * HEAD] = out[offset * rows : (offset + 1) * rows]
    count = kept_ref.shape[0] // 2
    copies[-1].wait()

    def block_of(peer):
        start = pl.multiple_of((me ^ peer) * count, count)
        return attended_ref[pl.ds(start, count), :]

    def project(one, other):
        return dot32(jnp.concatenate([block_of(one), block_of(other)], axis=0), weight_ref[...])

    sent_ref[...] = project(1, 3).astype(jnp.bfloat16)
    kept_ref[...] = project(0, 2)


def norm_kernel(experts_all, given, sources, results, arrival):
    stream_ref, payload_ref = results[:2]
    for copy in fetch(sources, results[2:], arrival):
        copy.wait()
    residual, kept, sibling, peer, gain, routes, gates = results[2:]
    rows, width = residual.shape
    stream = residual[...].astype(jnp.float32) + kept[:rows]
    stream = stream + sibling[:rows].astype(jnp.float32) + peer[...].astype(jnp.float32)
    stream_ref[...] = stream
    scale = lax.rsqrt(jnp.mean(stream * stream, axis=1, keepdims=True) + norm_eps)
    payload_ref[:, :width] = (stream * scale * gain[...]).astype(jnp.bfloat16)
    shape = (payload_ref.shape[1] - width, rows)
    lane = lax.broadcasted_iota(jnp.int32, shape, 0)
    expert = jnp.where(lane < experts_all, lane, lane - experts_all)
    dense = jnp.zeros(shape, jnp.float32)
    for copy in range(routes.shape[0]):
        chosen = routes[copy : copy + 1] == expert
        dense = dense + jnp.where(chosen, gates[copy : copy + 1], 0.0)
    high = dense.astype(jnp.bfloat16).astype(jnp.float32)
    spread = jnp.where(lane < experts_all, high, dense - high)
    payload_ref[:, width:] = spread.T.astype(jnp.bfloat16)


def slab_kernel(experts_all, given, sources, results, arrival):
    outs, refs = results[:4], results[4:]
    count = sources[0].shape[0]
    slab_ref, shared = refs[-1], refs[3:-1]
    gate_ref, up_ref, down_ref = given[1:] if len(given) > 1 else refs[:3]
    expert_ref = given[0]
    pieces = [slab_ref.at[pl.ds(index * count, count)] for index in range(4)]
    copies = fetch(sources, [*pieces, *refs[:-1]], arrival)
    for copy in copies[:4]:
        copy.wait()
    copies = copies[4:]
    width = outs[0].shape[1]
    rows = slab_ref[:, :width]
    tail = slab_ref[:, width:].astype(jnp.float32)
    lane = lax.broadcasted_iota(jnp.int32, tail.shape, 1)
    mine = (lane == expert_ref[0]) | (lane == expert_ref[0] + experts_all)
    weight = jnp.sum(jnp.where(mine, tail, 0.0), axis=1, keepdims=True)

    def arrived(ref):
        if copies:
            copies.pop(0).wait()
        return ref[...]

    def ffn(gate, up, down):
        gate_part = dot32(rows, arrived(gate))
        up_part = dot32(rows, arrived(up))
        hidden = (gate_part / (1.0 + jnp.exp(-gate_part)) * up_part).astype(jnp.bfloat16)
        return dot32(hidden, arrived(down)).astype(jnp.bfloat16).astype(jnp.float32)

    part = weight * ffn(gate_ref, up_ref, down_ref)
    if shared:
        part = part + ffn(*shared)
    for index, out in enumerate(outs):
        out[...] = part[index * count : (index + 1) * count].astype(out.dtype)


def on_core(kernel, name, outs, smem, placed, fetched, scratch, arguments):
    in_vmem = pl.BlockSpec(memory_space=pltpu.VMEM)
    fetched = [
        pltpu.with_memory_space_constraint(array, pltpu.HBM) if index in arguments else array
        for index, array in enumerate(fetched)
    ]
    inputs = len(smem) + len(placed) + len(fetched)
    first = inputs - len(fetched)

    def run(*refs):
        sources = refs[first:inputs]
        arrival = refs[-1]
        kernel(refs[: first], sources, refs[inputs:-1], arrival)

    return pl.pallas_call(
        run,
        out_shape=tuple(outs),
        in_specs=[pl.BlockSpec(memory_space=pltpu.SMEM)] * len(smem)
        + [in_vmem] * len(placed)
        + [pl.BlockSpec(memory_space=pl.ANY)] * len(fetched),
        out_specs=tuple(in_vmem for _ in outs),
        scratch_shapes=[*scratch, pltpu.SemaphoreType.DMA((len(fetched),))],
        compiler_params=pltpu.CompilerParams(vmem_limit_bytes=VMEM_BYTES),
        name=name,
    )(*smem, *placed, *fetched)


def fetch(sources, targets, arrival):
    copies = [
        pltpu.make_async_copy(source, target, arrival.at[index])
        for index, (source, target) in enumerate(zip(sources, targets))
    ]
    for copy in copies:
        copy.start()
    return copies


def room(array):
    return pltpu.VMEM(array.shape, array.dtype)


def flip(value, bit):
    count = lax.axis_size("tp")
    return lax.ppermute(value, "tp", [(i, i ^ bit) for i in range(count)])


def turn(value, step):
    count = lax.axis_size("sp")
    return lax.ppermute(value, "sp", [(i, (i + step) % count) for i in range(count)])


def neighbours(value):
    count = lax.axis_size("sp")
    even = [(i, i ^ 1) for i in range(count)]
    odd = [(i, later(i)) for i in range(1, count - 1)]
    return [lax.ppermute(value, "sp", pairs) for pairs in (even, odd)]


def gathered_layer(query_rows, key_rows, value_rows, sink_logit, operands):
    out_weight, residual, norm_gain, routes, gate_weights = operands[:5]
    expert_gate, expert_up, expert_down, shared_gate, shared_up, shared_down = operands[5:]
    count, width = residual.shape
    sp_count = lax.axis_size("sp")
    experts_all = sp_count * lax.axis_size("tp")
    here, me = lax.axis_index("sp"), lax.axis_index("tp")
    f32, bf16 = jnp.float32, jnp.bfloat16

    def held(rows, columns, dtype):
        return jax.ShapeDtypeStruct((rows, columns), dtype)

    local_len, kv_width = key_rows.shape
    near_keys, near_values = neighbours(key_rows), neighbours(value_rows)
    wide = pltpu.VMEM((3 * local_len, kv_width), bf16)
    kept, sent = on_core(
        functools.partial(attention_kernel, sp_count * local_len),
        "attention",
        [held(2 * count, width, f32), held(2 * count, width, bf16)],
        [
            jnp.stack([here, me]).astype(jnp.int32),
            pltpu.with_memory_space_constraint(sink_logit, pltpu.HBM),
        ],
        [],
        [query_rows, key_rows, *near_keys, value_rows, *near_values, out_weight],
        [room(query_rows), room(query_rows), wide, wide, room(out_weight)],
        (0, 1, 4, 7),
    )
    sibling = flip(sent, 1)
    peer = flip((kept[count:] + sibling[count:].astype(f32)).astype(bf16), 2)
    tail = 2 * experts_all + -(2 * experts_all) % LANES
    terms = [residual, kept, sibling, peer, norm_gain.reshape(1, width), routes.T, gate_weights.T]
    stream, payload = on_core(
        functools.partial(norm_kernel, experts_all),
        "norm",
        [held(count, width, f32), held(count, width + tail, bf16)],
        [],
        [],
        terms,
        [room(term) for term in terms],
        (0, 4, 5, 6),
    )

    expert = (here * lax.axis_size("tp") + me).reshape(1).astype(jnp.int32)
    halves = [held(count, width, f32)] * 2 + [held(count, width, bf16)] * 2
    slab_room = pltpu.VMEM((4 * count, width + tail), bf16)
    experts = [expert_gate[0], expert_up[0], expert_down[0]]
    shared = [shared_gate, shared_up, shared_down]

    def pieces_of(rows):
        crossed = flip(rows, 2)
        return [rows, crossed, flip(rows, 1), flip(crossed, 1)]

    def returned(kept, kept_cross, sent, sent_cross):
        kept_cross = (kept_cross + flip(sent_cross, 1).astype(f32)).astype(bf16)
        return kept + flip(sent, 1).astype(f32) + flip(kept_cross, 2).astype(f32)

    kernel = functools.partial(slab_kernel, experts_all)
    *own, gate, up, down = on_core(
        kernel,
        "own_slab",
        halves + [room(weights) for weights in experts],
        [expert],
        [],
        [*pieces_of(payload), *experts, *shared],
        [*[room(weights) for weights in shared], slab_room],
        range(4, 10),
    )
    total = stream
    for step in range(1, sp_count):
        parts = on_core(
            kernel,
            "slab",
            halves,
            [expert],
            [gate, up, down],
            pieces_of(turn(payload, step)),
            [slab_room],
            (),
        )
        total = total + turn(returned(*parts).astype(bf16), -step).astype(f32)
    total = total + returned(*own)
    return total.astype(bf16)


def body(query_rows, key_rows, value_rows, sink_logit, *operands):
    sp_count = lax.axis_size("sp")
    local_len = query_rows.shape[0]
    sent = 2 * operands[1].shape[0] * TOPK
    fits = lax.axis_size("tp") == 4 and sp_count % 2 == 0 and local_len == WINDOW
    if fits and 2 * sent >= sp_count * local_len:
        return gathered_layer(query_rows, key_rows, value_rows, sink_logit, operands)
    attended = window_attention(query_rows, key_rows, value_rows, sink_logit)
    return dispatched_layer(attended, operands)


def solution(mesh):
    placed = (
        P(("grp", "sp"), "tp"),
        P(("grp", "sp"), "tp"),
        P(("grp", "sp"), "tp"),
        P("tp"),
        P("tp", None),
        P(("grp", "sp", "tp"), None),
        P(),
        P(("grp", "sp", "tp"), None),
        P(("grp", "sp", "tp"), None),
        P(("sp", "tp"), None, None),
        P(("sp", "tp"), None, None),
        P(("sp", "tp"), None, None),
        P(None, "tp"),
        P(None, "tp"),
        P("tp", None),
    )
    return jax.shard_map(
        body, mesh=mesh, in_specs=placed, out_specs=P(("grp", "sp", "tp"), None), check_vma=False
    )
```

```python
import functools

import jax
import jax.numpy as jnp
from jax import lax
from jax.experimental import pallas as pl
from jax.experimental.pallas import tpu as pltpu
from jax.sharding import PartitionSpec as P

HEAD = 64
WINDOW = 128
TOPK = 6
LANES = 128
SLAB_WORK = 1 << 30
FILL_WORK = 1 << 31
VMEM_BYTES = 12 * 1024 * 1024

norm_eps = 1e-06


def with_halo(block, sides, width):
    for axis, dim in sides:
        count = lax.axis_size(axis)
        forward = [(i, i + 1) for i in range(count - 1)]
        backward = [(target, source) for source, target in forward]
        low = lax.ppermute(
            lax.slice_in_dim(block, block.shape[dim] - width, None, axis=dim), axis, forward
        )
        high = lax.ppermute(lax.slice_in_dim(block, 0, width, axis=dim), axis, backward)
        block = jnp.concatenate([low, block, high], axis=dim)
    return block


def window_attention(query_rows, key_rows, value_rows, sink_logit):
    local_len = query_rows.shape[0]
    head_size = HEAD
    local_kv = key_rows.shape[1] // head_size
    local_heads = query_rows.shape[1] // head_size
    grouped = local_heads // local_kv
    blocks = local_len // WINDOW
    stacked = jnp.stack([key_rows, value_rows])
    widened = with_halo(stacked, (("sp", 1),), WINDOW)
    banded = widened.reshape(2, blocks + 2, WINDOW, local_kv, head_size)
    banded = jnp.concatenate([banded[:, :-2], banded[:, 1:-1], banded[:, 2:]], axis=2)
    queries = query_rows.reshape(blocks, WINDOW, local_kv, grouped, head_size)
    scores = jnp.einsum(
        "nqhgd,nkhd->nhgqk", queries, banded[0], preferred_element_type=jnp.float32
    ) * head_size ** (-0.5)
    seq_start = lax.axis_index("sp") * local_len
    total_len = lax.axis_size("sp") * local_len
    block_ids = jnp.arange(blocks, dtype=jnp.int32)[:, None, None]
    query_pos = seq_start + block_ids * WINDOW + jnp.arange(WINDOW, dtype=jnp.int32)[None, :, None]
    key_pos = (
        seq_start
        + (block_ids - 1) * WINDOW
        + jnp.arange(3 * WINDOW, dtype=jnp.int32)[None, None, :]
    )
    in_window = (jnp.abs(key_pos - query_pos) <= WINDOW) & (key_pos >= 0) & (key_pos < total_len)
    scores = jnp.where(in_window[:, None, None], scores, -jnp.inf)
    sink_part = sink_logit.reshape(1, local_kv, grouped, 1, 1)
    row_max = jnp.maximum(sink_part, jnp.max(scores, axis=-1, keepdims=True))
    shifted = jnp.exp(scores - row_max)
    denominator = jnp.exp(sink_part - row_max) + jnp.sum(shifted, axis=-1, keepdims=True)
    weights = (shifted / denominator).astype(jnp.bfloat16)
    attended = jnp.einsum(
        "nhgqk,nkhd->nqhgd", weights, banded[1], preferred_element_type=jnp.float32
    )
    return attended.astype(jnp.bfloat16).reshape(local_len, local_heads * head_size)


def rms_norm(stream, norm_gain):
    return (
        stream * lax.rsqrt(jnp.mean(stream * stream, axis=-1, keepdims=True) + norm_eps) * norm_gain
    ).astype(jnp.bfloat16)


def gated(rows, gate, up):
    gate_part = jnp.dot(rows, gate, preferred_element_type=jnp.float32)
    up_part = jnp.dot(rows, up, preferred_element_type=jnp.float32)
    return (jax.nn.silu(gate_part) * up_part).astype(jnp.bfloat16)


def dispatched_layer(attended, operands):
    out_weight, residual, norm_gain, routes, gate_weights = operands[:5]
    expert_gate, expert_up, expert_down, shared_gate, shared_up, shared_down = operands[5:]
    tok_dev = attended.shape[0]
    tok_rows = residual.shape[0]
    model_width = residual.shape[1]
    projected = lax.psum_scatter(
        jnp.dot(attended, out_weight, preferred_element_type=jnp.float32).astype(jnp.bfloat16),
        "tp",
        scatter_dimension=0,
        tiled=True,
    ).astype(jnp.float32)
    stream = residual.astype(jnp.float32) + projected
    normed = rms_norm(stream, norm_gain)
    sp_count = lax.axis_size("sp")
    tp_count = lax.axis_size("tp")
    experts_all = sp_count * tp_count
    capacity = (2 * tok_dev * TOPK + tp_count * experts_all - 1) // (tp_count * experts_all)
    copies = tok_rows * TOPK
    flat_expert = routes.reshape(-1)
    one_hot = (flat_expert[:, None] == jnp.arange(experts_all, dtype=jnp.int32)[None, :]).astype(
        jnp.int32
    )
    rank_in_expert = jnp.sum(jnp.cumsum(one_hot, axis=0) * one_hot, axis=1) - 1
    target_slot = flat_expert * capacity + rank_in_expert
    slot_token = (
        jnp.full((experts_all * capacity,), tok_rows, jnp.int32)
        .at[target_slot]
        .set(jnp.arange(copies, dtype=jnp.int32) // TOPK)
    )
    padded_rows = jnp.concatenate([normed, jnp.zeros((1, model_width), jnp.bfloat16)], axis=0)
    outgoing = padded_rows[slot_token].reshape(experts_all, capacity, model_width)
    incoming = lax.all_to_all(outgoing, ("sp", "tp"), split_axis=0, concat_axis=0, tiled=True)
    hidden = gated(incoming.reshape(-1, model_width), expert_gate[0], expert_up[0])
    result = jnp.dot(hidden, expert_down[0], preferred_element_type=jnp.float32).astype(
        jnp.bfloat16
    )
    returned = lax.all_to_all(
        result.reshape(incoming.shape), ("sp", "tp"), split_axis=0, concat_axis=0, tiled=True
    )
    returned = returned.reshape(experts_all * capacity, model_width)
    gathered_copies = returned[target_slot].reshape(tok_rows, TOPK, model_width)
    routed = jnp.sum(gate_weights[:, :, None] * gathered_copies.astype(jnp.float32), axis=1)
    slab_rows = lax.all_gather(normed, "tp", axis=0, tiled=True)
    hidden = gated(slab_rows, shared_gate, shared_up)
    partials = jnp.dot(hidden, shared_down, preferred_element_type=jnp.float32)
    shared = lax.psum_scatter(
        partials.astype(jnp.bfloat16), "tp", scatter_dimension=0, tiled=True
    ).astype(jnp.float32)
    return (stream + routed + shared).astype(jnp.bfloat16)


def dot32(left, right):
    return jnp.dot(left, right, preferred_element_type=jnp.float32)


def later(index):
    return ((index + 1) ^ 1) - 1


def fill_kernel(given, sources, results, arrival):
    for copy in fetch(sources, results, arrival):
        copy.wait()


def pack_kernel(given, sources, results, arrival):
    rows = sources[0].shape[0]
    halves = [results[0].at[pl.ds(index * rows, rows)] for index in range(2)]
    fill_kernel(given, sources, halves, arrival)


def attention_kernel(total_len, given, sources, results, arrival):
    place_ref, sink_ref, query_ref, pack_ref, weight_ref = given
    kept_ref, sent_ref, attended_ref, *packs = results
    packs = [pack_ref, *packs]
    rows = query_ref.shape[0]
    copies = fetch(sources, packs[1:], arrival)
    heads = query_ref.shape[1] // HEAD
    kv_heads = pack_ref.shape[1] // HEAD
    grouped = heads // kv_heads
    here, me = place_ref[0], place_ref[1]
    span = (grouped * rows, 3 * rows)
    row = lax.broadcasted_iota(jnp.int32, span, 0)
    col = lax.broadcasted_iota(jnp.int32, span, 1)
    first = jnp.where(col < 2 * rows, ((here ^ 1) - 1) * rows, (later(here) - 2) * rows)
    key_pos = col + jnp.where(col < rows, here * rows, first)
    query_pos = here * rows + row % rows
    near = (jnp.abs(key_pos - query_pos) <= WINDOW) & (key_pos >= 0) & (key_pos < total_len)
    head_of = row[:, :1] // rows
    for copy in copies:
        copy.wait()
    keys = jnp.concatenate([pack[:rows] for pack in packs], axis=0)
    values = jnp.concatenate([pack[rows:] for pack in packs], axis=0)
    for group in range(kv_heads):
        lanes = slice(group * HEAD, (group + 1) * HEAD)
        first_head = group * grouped
        queries = jnp.concatenate(
            [
                query_ref[:, head * HEAD : (head + 1) * HEAD]
                for head in range(first_head, first_head + grouped)
            ],
            axis=0,
        )
        scores = lax.dot_general(
            queries, keys[:, lanes], (((1,), (1,)), ((), ())), preferred_element_type=jnp.float32
        )
        scores = jnp.where(near, scores * HEAD ** (-0.5), -jnp.inf)
        sink = jnp.full(head_of.shape, sink_ref[first_head], jnp.float32)
        for offset in range(1, grouped):
            sink = jnp.where(head_of == offset, sink_ref[first_head + offset], sink)
        row_max = jnp.maximum(sink, jnp.max(scores, axis=1, keepdims=True))
        shifted = jnp.exp(scores - row_max)
        denominator = jnp.exp(sink - row_max) + jnp.sum(shifted, axis=1, keepdims=True)
        weights = (shifted / denominator).astype(jnp.bfloat16)
        out = dot32(weights, values[:, lanes]).astype(jnp.bfloat16)
        for offset in range(grouped):
            head = first_head + offset
            attended_ref[:, head * HEAD : (head + 1) * HEAD] = out[offset * rows : (offset + 1) * rows]
    count = kept_ref.shape[0] // 2

    def block_of(peer):
        start = pl.multiple_of((me ^ peer) * count, count)
        return attended_ref[pl.ds(start, count), :]

    def project(one, other):
        return dot32(jnp.concatenate([block_of(one), block_of(other)], axis=0), weight_ref[...])

    sent_ref[...] = project(1, 3).astype(jnp.bfloat16)
    kept_ref[...] = project(0, 2)


def norm_kernel(experts_all, given, sources, results, arrival):
    stream_ref, payload_ref = results[:2]
    for copy in fetch(sources, results[2:], arrival):
        copy.wait()
    residual = given[0]
    kept, sibling, peer, gain, routes, gates = results[2:]
    rows, width = residual.shape
    stream = residual[...].astype(jnp.float32) + kept[:rows]
    stream = stream + sibling[:rows].astype(jnp.float32) + peer[...].astype(jnp.float32)
    stream_ref[...] = stream
    scale = lax.rsqrt(jnp.mean(stream * stream, axis=1, keepdims=True) + norm_eps)
    payload_ref[:, :width] = (stream * scale * gain[...]).astype(jnp.bfloat16)
    shape = (payload_ref.shape[1] - width, rows)
    lane = lax.broadcasted_iota(jnp.int32, shape, 0)
    expert = jnp.where(lane < experts_all, lane, lane - experts_all)
    dense = jnp.zeros(shape, jnp.float32)
    for copy in range(routes.shape[0]):
        chosen = routes[copy : copy + 1] == expert
        dense = dense + jnp.where(chosen, gates[copy : copy + 1], 0.0)
    high = dense.astype(jnp.bfloat16).astype(jnp.float32)
    spread = jnp.where(lane < experts_all, high, dense - high)
    payload_ref[:, width:] = spread.T.astype(jnp.bfloat16)


def slab_kernel(experts_all, given, sources, results, arrival):
    outs, refs = results[:4], results[4:]
    count = sources[0].shape[0]
    expert_ref, slab_ref = given[0], refs[-1]
    weights = given[1:] if len(given) > 1 else refs[:3]
    shared = refs[3:-1]
    pieces = [slab_ref.at[pl.ds(index * count, count)] for index in range(4)]
    copies = fetch(sources, [*pieces, *refs[:-1]], arrival)
    for copy in copies[:4]:
        copy.wait()
    coming = copies[4:]
    width = outs[0].shape[1]
    rows = slab_ref[:, :width]
    tail = slab_ref[:, width:].astype(jnp.float32)
    lane = lax.broadcasted_iota(jnp.int32, tail.shape, 1)
    mine = (lane == expert_ref[0]) | (lane == expert_ref[0] + experts_all)
    weight = jnp.sum(jnp.where(mine, tail, 0.0), axis=1, keepdims=True)

    def arrived(ref):
        if coming:
            coming.pop(0).wait()
        return ref[...]

    def ffn(gate, up, down):
        gate_part = dot32(rows, arrived(gate))
        up_part = dot32(rows, arrived(up))
        hidden = (gate_part / (1.0 + jnp.exp(-gate_part)) * up_part).astype(jnp.bfloat16)
        return dot32(hidden, arrived(down)).astype(jnp.bfloat16).astype(jnp.float32)

    part = weight * ffn(*weights)
    if shared:
        part = part + ffn(*shared)
    for index, out in enumerate(outs):
        out[...] = part[index * count : (index + 1) * count].astype(out.dtype)


def on_core(kernel, work, outs, smem, placed, fetched, scratch=(), arguments=()):
    in_vmem = pl.BlockSpec(memory_space=pltpu.VMEM)
    fetched = [
        pltpu.with_memory_space_constraint(array, pltpu.HBM) if index in arguments else array
        for index, array in enumerate(fetched)
    ]
    inputs = len(smem) + len(placed) + len(fetched)
    first = inputs - len(fetched)

    def run(*refs):
        sources = refs[first:inputs]
        arrival = refs[-1]
        kernel(refs[: first], sources, refs[inputs:-1], arrival)

    return pl.pallas_call(
        run,
        out_shape=tuple(outs),
        in_specs=[pl.BlockSpec(memory_space=pltpu.SMEM)] * len(smem)
        + [in_vmem] * len(placed)
        + [pl.BlockSpec(memory_space=pl.ANY)] * len(fetched),
        out_specs=tuple(in_vmem for _ in outs),
        scratch_shapes=[*scratch, pltpu.SemaphoreType.DMA((len(fetched),))],
        compiler_params=pltpu.CompilerParams(vmem_limit_bytes=VMEM_BYTES),
        cost_estimate=pl.CostEstimate(flops=work, transcendentals=0, bytes_accessed=0),
    )(*smem, *placed, *fetched)


def fetch(sources, targets, arrival):
    copies = [
        pltpu.make_async_copy(source, target, arrival.at[index])
        for index, (source, target) in enumerate(zip(sources, targets))
    ]
    for copy in copies:
        copy.start()
    return copies


def room(array):
    return pltpu.VMEM(array.shape, array.dtype)


def flip(value, bit):
    count = lax.axis_size("tp")
    return lax.ppermute(value, "tp", [(i, i ^ bit) for i in range(count)])


def swap(value, bits):
    count = lax.axis_size("sp")
    return lax.ppermute(value, "sp", [(i, i ^ bits) for i in range(count)])


def neighbours(value):
    count = lax.axis_size("sp")
    even = [(i, i ^ 1) for i in range(count)]
    odd = [(i, later(i)) for i in range(1, count - 1)]
    from_even = lax.ppermute(value, "sp", even)
    return [from_even, lax.ppermute(value, "sp", odd)]


def gathered_layer(query_rows, key_rows, value_rows, sink_logit, operands):
    out_weight, residual, norm_gain, routes, gate_weights = operands[:5]
    expert_gate, expert_up, expert_down, shared_gate, shared_up, shared_down = operands[5:]
    count, width = residual.shape
    sp_count = lax.axis_size("sp")
    experts_all = sp_count * lax.axis_size("tp")
    here, me = lax.axis_index("sp"), lax.axis_index("tp")
    f32, bf16 = jnp.float32, jnp.bfloat16

    def held(rows, columns, dtype):
        return jax.ShapeDtypeStruct((rows, columns), dtype)

    local_len, kv_width = key_rows.shape
    [pack] = on_core(
        pack_kernel,
        0,
        [pltpu.VMEM((2 * local_len, kv_width), bf16)],
        [],
        [],
        [key_rows, value_rows],
        arguments=(0, 1),
    )
    wanted = [query_rows, out_weight, residual]
    query_here, out_here, residual_here = on_core(
        fill_kernel, SLAB_WORK, [room(array) for array in wanted], [], [], wanted,
        arguments=(0, 1, 2),
    )

    kept, sent = on_core(
        functools.partial(attention_kernel, sp_count * local_len),
        SLAB_WORK,
        [held(2 * count, width, f32), held(2 * count, width, bf16)],
        [
            jnp.stack([here, me]).astype(jnp.int32),
            pltpu.with_memory_space_constraint(sink_logit, pltpu.HBM),
        ],
        [query_here, pack, out_here],
        neighbours(pack),
        [room(query_rows)] + [pltpu.VMEM((2 * local_len, kv_width), bf16)] * 2,
    )
    sibling = flip(sent, 1)
    peer = flip((kept[count:] + sibling[count:].astype(f32)).astype(bf16), 2)
    tail = 2 * experts_all + -(2 * experts_all) % LANES
    terms = [kept, sibling, peer, norm_gain.reshape(1, width), routes.T, gate_weights.T]
    stream, payload = on_core(
        functools.partial(norm_kernel, experts_all),
        SLAB_WORK // 2,
        [held(count, width, f32), held(count, width + tail, bf16)],
        [],
        [residual_here],
        terms,
        [room(term) for term in terms],
        (3, 4, 5),
    )

    expert = (here * lax.axis_size("tp") + me).reshape(1).astype(jnp.int32)
    halves = [held(count, width, f32)] * 2 + [held(count, width, bf16)] * 2

    experts = [expert_gate[0], expert_up[0], expert_down[0]]
    shared = [shared_gate, shared_up, shared_down]
    slab_room = pltpu.VMEM((4 * count, width + tail), bf16)

    def pieces_of(rows):
        crossed = flip(rows, 2)
        return [rows, crossed, flip(rows, 1), flip(crossed, 1)]

    def returned(kept, kept_cross, sent, sent_cross):
        sent_cross = flip(sent_cross, 1)
        kept_cross = (kept_cross + sent_cross.astype(f32)).astype(bf16)
        sent = flip(sent, 1)
        return kept + sent.astype(f32) + flip(kept_cross, 2).astype(f32)

    kernel = functools.partial(slab_kernel, experts_all)
    *own, gate, up, down = on_core(
        kernel,
        FILL_WORK,
        halves + [room(array) for array in experts],
        [expert],
        [],
        [*pieces_of(payload), *experts, *shared],
        [*[room(array) for array in shared], slab_room],
        range(4, 10),
    )
    total = stream + returned(*own)
    for step in range(1, sp_count):
        parts = on_core(
            kernel,
            SLAB_WORK,
            halves,
            [expert],
            [gate, up, down],
            pieces_of(swap(payload, step)),
            [slab_room],
        )
        part = returned(*parts).astype(bf16)
        total = total + swap(part, step).astype(f32)
    return total.astype(bf16)


def body(query_rows, key_rows, value_rows, sink_logit, *operands):
    sp_count = lax.axis_size("sp")
    local_len = query_rows.shape[0]
    sent = 2 * operands[1].shape[0] * TOPK
    fits = lax.axis_size("tp") == 4 and sp_count & (sp_count - 1) == 0 and local_len == WINDOW
    if fits and 2 * sent >= sp_count * local_len:
        return gathered_layer(query_rows, key_rows, value_rows, sink_logit, operands)
    attended = window_attention(query_rows, key_rows, value_rows, sink_logit)
    return dispatched_layer(attended, operands)


def solution(mesh):
    placed = (
        P(("grp", "sp"), "tp"),
        P(("grp", "sp"), "tp"),
        P(("grp", "sp"), "tp"),
        P("tp"),
        P("tp", None),
        P(("grp", "sp", "tp"), None),
        P(),
        P(("grp", "sp", "tp"), None),
        P(("grp", "sp", "tp"), None),
        P(("sp", "tp"), None, None),
        P(("sp", "tp"), None, None),
        P(("sp", "tp"), None, None),
        P(None, "tp"),
        P(None, "tp"),
        P("tp", None),
    )
    return jax.shard_map(
        body, mesh=mesh, in_specs=placed, out_specs=P(("grp", "sp", "tp"), None), check_vma=False
    )
```

```python
import functools

import jax
import jax.numpy as jnp
from jax import lax
from jax.experimental import pallas as pl
from jax.experimental.pallas import tpu as pltpu
from jax.sharding import PartitionSpec as P

HEAD = 64
WINDOW = 128
TOPK = 6
LANES = 128
SLAB_WORK = 1 << 30
FILL_WORK = 1 << 31
VMEM_BYTES = 12 * 1024 * 1024

norm_eps = 1e-06


def with_halo(block, sides, width):
    for axis, dim in sides:
        count = lax.axis_size(axis)
        forward = [(i, i + 1) for i in range(count - 1)]
        backward = [(target, source) for source, target in forward]
        low = lax.ppermute(
            lax.slice_in_dim(block, block.shape[dim] - width, None, axis=dim), axis, forward
        )
        high = lax.ppermute(lax.slice_in_dim(block, 0, width, axis=dim), axis, backward)
        block = jnp.concatenate([low, block, high], axis=dim)
    return block


def window_attention(query_rows, key_rows, value_rows, sink_logit):
    local_len = query_rows.shape[0]
    head_size = HEAD
    local_kv = key_rows.shape[1] // head_size
    local_heads = query_rows.shape[1] // head_size
    grouped = local_heads // local_kv
    blocks = local_len // WINDOW
    stacked = jnp.stack([key_rows, value_rows])
    widened = with_halo(stacked, (("sp", 1),), WINDOW)
    banded = widened.reshape(2, blocks + 2, WINDOW, local_kv, head_size)
    banded = jnp.concatenate([banded[:, :-2], banded[:, 1:-1], banded[:, 2:]], axis=2)
    queries = query_rows.reshape(blocks, WINDOW, local_kv, grouped, head_size)
    scores = jnp.einsum(
        "nqhgd,nkhd->nhgqk", queries, banded[0], preferred_element_type=jnp.float32
    ) * head_size ** (-0.5)
    seq_start = lax.axis_index("sp") * local_len
    total_len = lax.axis_size("sp") * local_len
    block_ids = jnp.arange(blocks, dtype=jnp.int32)[:, None, None]
    query_pos = seq_start + block_ids * WINDOW + jnp.arange(WINDOW, dtype=jnp.int32)[None, :, None]
    key_pos = (
        seq_start
        + (block_ids - 1) * WINDOW
        + jnp.arange(3 * WINDOW, dtype=jnp.int32)[None, None, :]
    )
    in_window = (jnp.abs(key_pos - query_pos) <= WINDOW) & (key_pos >= 0) & (key_pos < total_len)
    scores = jnp.where(in_window[:, None, None], scores, -jnp.inf)
    sink_part = sink_logit.reshape(1, local_kv, grouped, 1, 1)
    row_max = jnp.maximum(sink_part, jnp.max(scores, axis=-1, keepdims=True))
    shifted = jnp.exp(scores - row_max)
    denominator = jnp.exp(sink_part - row_max) + jnp.sum(shifted, axis=-1, keepdims=True)
    weights = (shifted / denominator).astype(jnp.bfloat16)
    attended = jnp.einsum(
        "nhgqk,nkhd->nqhgd", weights, banded[1], preferred_element_type=jnp.float32
    )
    return attended.astype(jnp.bfloat16).reshape(local_len, local_heads * head_size)


def rms_norm(stream, norm_gain):
    return (
        stream * lax.rsqrt(jnp.mean(stream * stream, axis=-1, keepdims=True) + norm_eps) * norm_gain
    ).astype(jnp.bfloat16)


def gated(rows, gate, up):
    gate_part = jnp.dot(rows, gate, preferred_element_type=jnp.float32)
    up_part = jnp.dot(rows, up, preferred_element_type=jnp.float32)
    return (jax.nn.silu(gate_part) * up_part).astype(jnp.bfloat16)


def dispatched_layer(attended, operands):
    out_weight, residual, norm_gain, routes, gate_weights = operands[:5]
    expert_gate, expert_up, expert_down, shared_gate, shared_up, shared_down = operands[5:]
    tok_dev = attended.shape[0]
    tok_rows = residual.shape[0]
    model_width = residual.shape[1]
    projected = lax.psum_scatter(
        jnp.dot(attended, out_weight, preferred_element_type=jnp.float32).astype(jnp.bfloat16),
        "tp",
        scatter_dimension=0,
        tiled=True,
    ).astype(jnp.float32)
    stream = residual.astype(jnp.float32) + projected
    normed = rms_norm(stream, norm_gain)
    sp_count = lax.axis_size("sp")
    tp_count = lax.axis_size("tp")
    experts_all = sp_count * tp_count
    capacity = (2 * tok_dev * TOPK + tp_count * experts_all - 1) // (tp_count * experts_all)
    copies = tok_rows * TOPK
    flat_expert = routes.reshape(-1)
    one_hot = (flat_expert[:, None] == jnp.arange(experts_all, dtype=jnp.int32)[None, :]).astype(
        jnp.int32
    )
    rank_in_expert = jnp.sum(jnp.cumsum(one_hot, axis=0) * one_hot, axis=1) - 1
    target_slot = flat_expert * capacity + rank_in_expert
    slot_token = (
        jnp.full((experts_all * capacity,), tok_rows, jnp.int32)
        .at[target_slot]
        .set(jnp.arange(copies, dtype=jnp.int32) // TOPK)
    )
    padded_rows = jnp.concatenate([normed, jnp.zeros((1, model_width), jnp.bfloat16)], axis=0)
    outgoing = padded_rows[slot_token].reshape(experts_all, capacity, model_width)
    incoming = lax.all_to_all(outgoing, ("sp", "tp"), split_axis=0, concat_axis=0, tiled=True)
    hidden = gated(incoming.reshape(-1, model_width), expert_gate[0], expert_up[0])
    result = jnp.dot(hidden, expert_down[0], preferred_element_type=jnp.float32).astype(
        jnp.bfloat16
    )
    returned = lax.all_to_all(
        result.reshape(incoming.shape), ("sp", "tp"), split_axis=0, concat_axis=0, tiled=True
    )
    returned = returned.reshape(experts_all * capacity, model_width)
    gathered_copies = returned[target_slot].reshape(tok_rows, TOPK, model_width)
    routed = jnp.sum(gate_weights[:, :, None] * gathered_copies.astype(jnp.float32), axis=1)
    slab_rows = lax.all_gather(normed, "tp", axis=0, tiled=True)
    hidden = gated(slab_rows, shared_gate, shared_up)
    partials = jnp.dot(hidden, shared_down, preferred_element_type=jnp.float32)
    shared = lax.psum_scatter(
        partials.astype(jnp.bfloat16), "tp", scatter_dimension=0, tiled=True
    ).astype(jnp.float32)
    return (stream + routed + shared).astype(jnp.bfloat16)


def dot32(left, right):
    return jnp.dot(left, right, preferred_element_type=jnp.float32)


def later(index):
    return ((index + 1) ^ 1) - 1


def fill_kernel(given, sources, results, arrival):
    copies = fetch(sources, results, arrival)
    if given:
        sinks_ref = results[-1]
        for head in range(sinks_ref.shape[0]):
            sinks_ref[head : head + 1] = jnp.full((1, sinks_ref.shape[1]), given[0][head])
    for copy in copies:
        copy.wait()


def pack_kernel(given, sources, results, arrival):
    rows = sources[0].shape[0]
    halves = [results[0].at[pl.ds(index * rows, rows)] for index in range(2)]
    fill_kernel(given, sources, halves, arrival)


def attention_kernel(total_len, given, sources, results, arrival):
    query_ref, weight_ref, sinks_ref, *packs = given
    kept_ref, sent_ref, attended_ref = results
    rows = query_ref.shape[0]
    heads = query_ref.shape[1] // HEAD
    kv_heads = packs[0].shape[1] // HEAD
    grouped = heads // kv_heads
    here, me = lax.axis_index("sp"), lax.axis_index("tp")
    span = (grouped * rows, 3 * rows)
    row = lax.broadcasted_iota(jnp.int32, span, 0)
    col = lax.broadcasted_iota(jnp.int32, span, 1)
    first = jnp.where(col < 2 * rows, ((here ^ 1) - 1) * rows, (later(here) - 2) * rows)
    key_pos = col + jnp.where(col < rows, here * rows, first)
    query_pos = here * rows + row % rows
    near = (jnp.abs(key_pos - query_pos) <= WINDOW) & (key_pos >= 0) & (key_pos < total_len)
    head_of = row[:, :1] // rows
    keys = jnp.concatenate([pack[:rows] for pack in packs], axis=0)
    values = jnp.concatenate([pack[rows:] for pack in packs], axis=0)
    for group in range(kv_heads):
        lanes = slice(group * HEAD, (group + 1) * HEAD)
        first_head = group * grouped
        queries = jnp.concatenate(
            [
                query_ref[:, head * HEAD : (head + 1) * HEAD]
                for head in range(first_head, first_head + grouped)
            ],
            axis=0,
        )
        scores = lax.dot_general(
            queries, keys[:, lanes], (((1,), (1,)), ((), ())), preferred_element_type=jnp.float32
        )
        scores = jnp.where(near, scores * HEAD ** (-0.5), -jnp.inf)
        sink = jnp.broadcast_to(sinks_ref[first_head : first_head + 1, :1], head_of.shape)
        for offset in range(1, grouped):
            head = first_head + offset
            sink = jnp.where(head_of == offset, sinks_ref[head : head + 1, :1], sink)
        row_max = jnp.maximum(sink, jnp.max(scores, axis=1, keepdims=True))
        shifted = jnp.exp(scores - row_max)
        denominator = jnp.exp(sink - row_max) + jnp.sum(shifted, axis=1, keepdims=True)
        weights = (shifted / denominator).astype(jnp.bfloat16)
        out = dot32(weights, values[:, lanes]).astype(jnp.bfloat16)
        for offset in range(grouped):
            head = first_head + offset
            attended_ref[:, head * HEAD : (head + 1) * HEAD] = out[offset * rows : (offset + 1) * rows]
    count = kept_ref.shape[0] // 2

    def block_of(peer):
        start = pl.multiple_of((me ^ peer) * count, count)
        return attended_ref[pl.ds(start, count), :]

    def project(one, other):
        return dot32(jnp.concatenate([block_of(one), block_of(other)], axis=0), weight_ref[...])

    sent_ref[...] = project(1, 3).astype(jnp.bfloat16)
    kept_ref[...] = project(0, 2)


def norm_kernel(experts_all, given, sources, results, arrival):
    stream_ref, payload_ref = results
    residual, gain, routes, gates, kept, sibling, peer = given
    rows, width = residual.shape
    stream = residual[...].astype(jnp.float32) + kept[:rows]
    stream = stream + sibling[:rows].astype(jnp.float32) + peer[...].astype(jnp.float32)
    stream_ref[...] = stream
    scale = lax.rsqrt(jnp.mean(stream * stream, axis=1, keepdims=True) + norm_eps)
    payload_ref[:, :width] = (stream * scale * gain[...]).astype(jnp.bfloat16)
    shape = (payload_ref.shape[1] - width, rows)
    lane = lax.broadcasted_iota(jnp.int32, shape, 0)
    expert = jnp.where(lane < experts_all, lane, lane - experts_all)
    dense = jnp.zeros(shape, jnp.float32)
    for copy in range(routes.shape[0]):
        chosen = routes[copy : copy + 1] == expert
        dense = dense + jnp.where(chosen, gates[copy : copy + 1], 0.0)
    high = dense.astype(jnp.bfloat16).astype(jnp.float32)
    spread = jnp.where(lane < experts_all, high, dense - high)
    payload_ref[:, width:] = spread.T.astype(jnp.bfloat16)


def slab_kernel(tp_count, experts_all, given, sources, results, arrival):
    kept_ref, kept_cross_ref, sent_ref, slab_ref = results
    pieces, weights, shared = given[:4], given[4:7], given[7:]
    count, width = kept_ref.shape
    for index, piece in enumerate(pieces):
        slab_ref[index * count : (index + 1) * count] = piece[...]
    expert = lax.axis_index("sp") * tp_count + lax.axis_index("tp")
    rows = slab_ref[:, :width]
    tail = slab_ref[:, width:].astype(jnp.float32)
    lane = lax.broadcasted_iota(jnp.int32, tail.shape, 1)
    mine = (lane == expert) | (lane == expert + experts_all)
    weight = jnp.sum(jnp.where(mine, tail, 0.0), axis=1, keepdims=True)

    def ffn(gate, up, down):
        gate_part = dot32(rows, gate[...])
        up_part = dot32(rows, up[...])
        hidden = (gate_part / (1.0 + jnp.exp(-gate_part)) * up_part).astype(jnp.bfloat16)
        return dot32(hidden, down[...]).astype(jnp.bfloat16).astype(jnp.float32)

    part = weight * ffn(*weights)
    if shared:
        part = part + ffn(*shared)
    kept_ref[...] = part[:count]
    kept_cross_ref[...] = part[count : 2 * count]
    sent_ref[...] = part[2 * count :].astype(jnp.bfloat16)


def on_core(kernel, work, outs, smem, placed, fetched, scratch=(), arguments=()):
    in_vmem = pl.BlockSpec(memory_space=pltpu.VMEM)
    fetched = [
        pltpu.with_memory_space_constraint(array, pltpu.HBM) if index in arguments else array
        for index, array in enumerate(fetched)
    ]
    inputs = len(smem) + len(placed) + len(fetched)
    first = inputs - len(fetched)

    def run(*refs):
        sources = refs[first:inputs]
        arrival = refs[-1]
        kernel(refs[: first], sources, refs[inputs:-1], arrival)

    return pl.pallas_call(
        run,
        out_shape=tuple(outs),
        in_specs=[pl.BlockSpec(memory_space=pltpu.SMEM)] * len(smem)
        + [in_vmem] * len(placed)
        + [pl.BlockSpec(memory_space=pl.ANY)] * len(fetched),
        out_specs=tuple(in_vmem for _ in outs),
        scratch_shapes=[*scratch, pltpu.SemaphoreType.DMA((max(len(fetched), 1),))],
        compiler_params=pltpu.CompilerParams(vmem_limit_bytes=VMEM_BYTES),
        cost_estimate=pl.CostEstimate(flops=work, transcendentals=0, bytes_accessed=0),
    )(*smem, *placed, *fetched)


def fetch(sources, targets, arrival):
    copies = [
        pltpu.make_async_copy(source, target, arrival.at[index])
        for index, (source, target) in enumerate(zip(sources, targets))
    ]
    for copy in copies:
        copy.start()
    return copies


def room(array):
    return pltpu.VMEM(array.shape, array.dtype)


def flip(value, bit):
    count = lax.axis_size("tp")
    return lax.ppermute(value, "tp", [(i, i ^ bit) for i in range(count)])


def swap(value, bits):
    count = lax.axis_size("sp")
    return lax.ppermute(value, "sp", [(i, i ^ bits) for i in range(count)])


def neighbours(value):
    count = lax.axis_size("sp")
    even = [(i, i ^ 1) for i in range(count)]
    odd = [(i, later(i)) for i in range(1, count - 1)]
    from_even = lax.ppermute(value, "sp", even)
    return [from_even, lax.ppermute(value, "sp", odd)]


def gathered_layer(query_rows, key_rows, value_rows, sink_logit, operands):
    out_weight, residual, norm_gain, routes, gate_weights = operands[:5]
    expert_gate, expert_up, expert_down, shared_gate, shared_up, shared_down = operands[5:]
    count, width = residual.shape
    sp_count = lax.axis_size("sp")
    experts_all = sp_count * lax.axis_size("tp")
    f32, bf16 = jnp.float32, jnp.bfloat16

    def held(rows, columns, dtype):
        return jax.ShapeDtypeStruct((rows, columns), dtype)

    local_len, kv_width = key_rows.shape
    [pack] = on_core(
        pack_kernel,
        0,
        [pltpu.VMEM((2 * local_len, kv_width), bf16)],
        [],
        [],
        [key_rows, value_rows],
        arguments=(0, 1),
    )
    wanted = [query_rows, out_weight, residual, norm_gain.reshape(1, width)]
    wanted += [routes.T, gate_weights.T, expert_gate[0], expert_up[0], expert_down[0]]
    wanted += [shared_gate, shared_up, shared_down]
    query_here, out_here, *filled = on_core(
        fill_kernel,
        FILL_WORK,
        [*[room(array) for array in wanted], pltpu.VMEM((sink_logit.shape[0], LANES), f32)],
        [pltpu.with_memory_space_constraint(sink_logit, pltpu.HBM)],
        [],
        wanted,
        arguments=range(len(wanted)),
    )
    terms, weights, shared, sinks = filled[:4], filled[4:7], filled[7:10], filled[10]

    kept, sent = on_core(
        functools.partial(attention_kernel, sp_count * local_len),
        SLAB_WORK,
        [held(2 * count, width, f32), held(2 * count, width, bf16)],
        [],
        [query_here, out_here, sinks, pack, *neighbours(pack)],
        [],
        [room(query_rows)],
    )
    sibling = flip(sent, 1)
    peer = flip((kept[count:] + sibling[count:].astype(f32)).astype(bf16), 2)
    tail = 2 * experts_all + -(2 * experts_all) % LANES
    stream, payload = on_core(
        functools.partial(norm_kernel, experts_all),
        SLAB_WORK // 2,
        [held(count, width, f32), held(count, width + tail, bf16)],
        [],
        [*terms, kept, sibling, peer],
        [],
    )

    halves = [held(count, width, f32)] * 2 + [held(2 * count, width, bf16)]

    slab_room = pltpu.VMEM((4 * count, width + tail), bf16)

    def pieces_of(rows):
        crossed = flip(rows, 2)
        return [rows, crossed, flip(rows, 1), flip(crossed, 1)]

    def returned(kept, kept_cross, sent):
        sent = flip(sent, 1).astype(f32)
        kept_cross = (kept_cross + sent[count:]).astype(bf16)
        return kept + sent[:count] + flip(kept_cross, 2).astype(f32)

    def through_expert(rows, *shared):
        parts = on_core(
            functools.partial(slab_kernel, lax.axis_size("tp"), experts_all),
            SLAB_WORK,
            halves,
            [],
            [*pieces_of(rows), *weights, *shared],
            [],
            [slab_room],
        )
        return returned(*parts)

    total = stream + through_expert(payload, *shared)
    for step in range(1, sp_count):
        part = through_expert(swap(payload, step)).astype(bf16)
        total = total + swap(part, step).astype(f32)
    return total.astype(bf16)


def body(query_rows, key_rows, value_rows, sink_logit, *operands):
    sp_count = lax.axis_size("sp")
    local_len = query_rows.shape[0]
    sent = 2 * operands[1].shape[0] * TOPK
    fits = lax.axis_size("tp") == 4 and sp_count & (sp_count - 1) == 0 and local_len == WINDOW
    if fits and 2 * sent >= sp_count * local_len:
        return gathered_layer(query_rows, key_rows, value_rows, sink_logit, operands)
    attended = window_attention(query_rows, key_rows, value_rows, sink_logit)
    return dispatched_layer(attended, operands)


def solution(mesh):
    placed = (
        P(("grp", "sp"), "tp"),
        P(("grp", "sp"), "tp"),
        P(("grp", "sp"), "tp"),
        P("tp"),
        P("tp", None),
        P(("grp", "sp", "tp"), None),
        P(),
        P(("grp", "sp", "tp"), None),
        P(("grp", "sp", "tp"), None),
        P(("sp", "tp"), None, None),
        P(("sp", "tp"), None, None),
        P(("sp", "tp"), None, None),
        P(None, "tp"),
        P(None, "tp"),
        P("tp", None),
    )
    return jax.shard_map(
        body, mesh=mesh, in_specs=placed, out_specs=P(("grp", "sp", "tp"), None), check_vma=False
    )
```
